128 devices in a mesh: fs: 16 (over z, y), tp: 8 (over x, core).
Axes of the slice: x: 4, y: 4, z: 4, core: 2. Of those that a mesh axis runs over, the one named last changes fastest.
Arguments:
- tokens: bfloat16 [16, 384, 2048], P('fs', None, 'tp'), may hold values from -16 to 16
- first_gate: bfloat16 [2048, 6144], P('fs', 'tp'), may hold values from -0.125 to 0.125
- first_up: bfloat16 [2048, 6144], P('fs', 'tp'), may hold values from -0.125 to 0.125
- first_down: bfloat16 [6144, 2048], P('tp', 'fs'), may hold values from -0.078125 to 0.078125
- first_gain: bfloat16 [2048], P('tp'), may hold values from 0.099609375 to 1.8984375
- glu_value: bfloat16 [2048, 1024], P('fs', 'tp'), may hold values from -0.125 to 0.125
- glu_gate: bfloat16 [2048, 1024], P('fs', 'tp'), may hold values from -0.125 to 0.125
- conv_taps: bfloat16 [31, 1024], P(None, 'tp'), may hold values from -3 to 3
- conv_gain: bfloat16 [1024], P('tp'), may hold values from 0.099609375 to 1.8984375
- conv_proj: bfloat16 [1024, 2048], P('tp', 'fs'), may hold values from -0.1875 to 0.1875
- second_gain: bfloat16 [2048], P('tp'), may hold values from 0.099609375 to 1.8984375
- last_gate: bfloat16 [2048, 6144], P('fs', 'tp'), may hold values from -0.125 to 0.125
- last_up: bfloat16 [2048, 6144], P('fs', 'tp'), may hold values from -0.125 to 0.125
- last_down: bfloat16 [6144, 2048], P('tp', 'fs'), may hold values from -0.078125 to 0.078125
- third_gain: bfloat16 [2048], P('tp'), may hold values from 0.099609375 to 1.8984375
Outputs:
- layer_out: bfloat16 [16, 384, 2048], P('fs', None, 'tp')
The draws below stay inside these ranges and needn't reach their ends.
All inputs are finite; a program needn't handle non-finite values.
Results may differ from the reference program's by a relative error of at most 0.015.
Values may be sent and summed in bfloat16 or wider, within the bound.
No kernel may reach another device: no remote copies, remote signals or barrier semaphores. Data moves between devices by JAX's collectives and lax.ppermute only.
A program may use at most 64 MiB of HBM per device.

```python
import jax
import jax.numpy as jnp
from jax import lax

D = 2048
FF = 6144
CONV = 1024
KERNEL = 31
LEN = 384
SEQS = 16
N_TP = 8


def draw_tokens(key, part):
    values = jnp.clip(jax.random.normal(key, (SEQS, LEN, D), jnp.float32), -5.0, 5.0)
    rising = 10.0 ** (jnp.arange(D, dtype=jnp.float32) / D - 0.5)
    return (values * rising).astype(jnp.bfloat16)


def draw_conv_taps(key, part):
    values = jnp.clip(jax.random.normal(key, (KERNEL, CONV), jnp.float32), -5.0, 5.0)
    rising = 10.0 ** (jnp.arange(CONV, dtype=jnp.float32) / CONV - 0.5)
    return (values * rising / jnp.sqrt(1.0 * KERNEL)).astype(jnp.bfloat16)


def shard_levels(own_key, extent, pieces, low, high):
    level, own = 1.0, jax.random.fold_in(own_key, 6)
    for axis_at, blocks in pieces:
        heights = jnp.exp(jax.random.uniform(jax.random.fold_in(own, axis_at), (blocks,), jnp.float32, low / len(pieces), high / len(pieces)))
        level = level * jnp.repeat(heights, extent[axis_at] // blocks).reshape([-1 if axis == axis_at else 1 for axis in range(len(extent))])
    return level


def centred(stream_key, extent, scale, bound, pieces=(), kind=jnp.bfloat16):
    values = scale * jax.random.normal(stream_key, extent, jnp.float32)
    if pieces:
        values = values * shard_levels(stream_key, extent, pieces, -0.22, 0.18)
    return jnp.clip(values, -bound, bound).astype(kind)


def setup_inputs(seed: int = 0) -> dict:
    streams_of = jax.random.split(jax.random.key(seed), 16)
    tokens = draw_tokens(jax.random.fold_in(streams_of[15], 71), 0)
    first_gate = centred(streams_of[1], (D, FF), D ** -0.5, 0.125, ((0, 16), (1, 8)))
    first_up = centred(streams_of[2], (D, FF), D ** -0.5, 0.125, ((0, 16), (1, 8)))
    first_down = centred(streams_of[3], (FF, D), FF ** -0.5, 0.078125, ((0, 8), (1, 16)))
    first_gain = jnp.clip(1.0 + 0.18 * jax.random.normal(streams_of[4], (D,), jnp.float32), 0.099609375, 1.8984375).astype(jnp.bfloat16)
    glu_value = centred(streams_of[5], (D, CONV), D ** -0.5, 0.125, ((0, 16), (1, 8)))
    glu_gate = centred(streams_of[6], (D, CONV), D ** -0.5, 0.125, ((0, 16), (1, 8)))
    conv_taps = draw_conv_taps(jax.random.fold_in(streams_of[15], 71), 0)
    conv_gain = jnp.clip(1.0 + 0.18 * jax.random.normal(streams_of[8], (CONV,), jnp.float32), 0.099609375, 1.8984375).astype(jnp.bfloat16)
    conv_proj = centred(streams_of[9], (CONV, D), CONV ** -0.5, 0.1875, ((0, 8), (1, 16)))
    second_gain = jnp.clip(1.0 + 0.18 * jax.random.normal(streams_of[10], (D,), jnp.float32), 0.099609375, 1.8984375).astype(jnp.bfloat16)
    last_gate = centred(streams_of[11], (D, FF), D ** -0.5, 0.125, ((0, 16), (1, 8)))
    last_up = centred(streams_of[12], (D, FF), D ** -0.5, 0.125, ((0, 16), (1, 8)))
    last_down = centred(streams_of[13], (FF, D), FF ** -0.5, 0.078125, ((0, 8), (1, 16)))
    third_gain = jnp.clip(1.0 + 0.18 * jax.random.normal(streams_of[14], (D,), jnp.float32), 0.099609375, 1.8984375).astype(jnp.bfloat16)
    return dict(tokens=tokens, first_gate=first_gate, first_up=first_up, first_down=first_down, first_gain=first_gain, glu_value=glu_value, glu_gate=glu_gate, conv_taps=conv_taps, conv_gain=conv_gain, conv_proj=conv_proj, second_gain=second_gain, last_gate=last_gate, last_up=last_up, last_down=last_down, third_gain=third_gain)


ALPHA = 2.0 ** 0.25
EPSILON = 1e-05

def norm_rows(values, gain):
    center = lax.optimization_barrier(jnp.mean(values, axis=-1, keepdims=True))
    spread = lax.optimization_barrier(jnp.mean(jnp.square(values - center), axis=-1, keepdims=True))
    return (values - center) * lax.rsqrt(spread + EPSILON) * gain.astype(jnp.float32)

def split_sum(hidden, weight):
    blocks = hidden.shape[1] // N_TP
    left = hidden.reshape(hidden.shape[0], N_TP, blocks).astype(jnp.float32)
    right = weight.reshape(N_TP, blocks, weight.shape[1]).astype(jnp.float32)
    parts = jnp.einsum('rbf,bfd->brd', left, right)
    parts = lax.optimization_barrier(parts.astype(jnp.bfloat16))
    return lax.optimization_barrier(jnp.sum(parts.astype(jnp.float32), axis=0))

def feed_forward(current, w_gate, w_up, w_down):
    gate = jnp.dot(current, w_gate, preferred_element_type=jnp.float32)
    upward = jnp.dot(current, w_up, preferred_element_type=jnp.float32)
    hidden = (jax.nn.silu(gate) * upward).astype(jnp.bfloat16)
    return split_sum(hidden, w_down)

def post_norm(current, branch, weight, gain):
    mixed = ALPHA * current.astype(jnp.float32) + weight * branch
    return norm_rows(mixed, gain).astype(jnp.bfloat16)

def conv_module(current, glu_value, glu_gate, conv_taps, conv_gain, conv_proj):
    value = jnp.dot(current, glu_value, preferred_element_type=jnp.float32)
    gate = jnp.dot(current, glu_gate, preferred_element_type=jnp.float32)
    gated = value * jax.nn.sigmoid(gate)
    reach = (conv_taps.shape[0] - 1) // 2
    length = gated.shape[0]
    padded = jnp.pad(gated, ((reach, reach), (0, 0)))
    taps = conv_taps.astype(jnp.float32)
    mixed = jnp.zeros_like(gated)
    for tap_index in range(conv_taps.shape[0]):
        mixed = mixed + taps[tap_index] * padded[tap_index:tap_index + length]
    normed = jax.nn.silu(norm_rows(mixed, conv_gain)).astype(jnp.bfloat16)
    return split_sum(normed, conv_proj)

def reference(tokens, first_gate, first_up, first_down, first_gain, glu_value, glu_gate, conv_taps, conv_gain, conv_proj, second_gain, last_gate, last_up, last_down, third_gain):

    def one_sequence(current):
        first = post_norm(current, feed_forward(current, first_gate, first_up, first_down), 0.5, first_gain)
        second = post_norm(first, conv_module(first, glu_value, glu_gate, conv_taps, conv_gain, conv_proj), 1.0, second_gain)
        return post_norm(second, feed_forward(second, last_gate, last_up, last_down), 0.5, third_gain)
    return lax.map(one_sequence, tokens)
```

```python
import jax
import jax.numpy as jnp
from jax import lax
from jax.sharding import PartitionSpec as P

ALPHA = 2.0**0.25
EPSILON = 1e-05
F32 = jnp.float32
BF16 = jnp.bfloat16


def pull(value, axis, distance):
    if axis == "z":
        pairs = [(i, ((i // 4 - distance) % 4) * 4 + i % 4) for i in range(16)]
    elif axis == "y":
        pairs = [(i, (i // 4) * 4 + (i % 4 - distance) % 4) for i in range(16)]
    elif axis == "x":
        pairs = [(i, ((i // 2 - distance) % 4) * 2 + i % 2) for i in range(8)]
    else:
        pairs = [(i, i ^ 1) for i in range(8)]
    return lax.ppermute(value, "fs" if axis in "zy" else "tp", pairs)


def neighbours(value, axis):
    return pull(value, axis, 1), pull(value, axis, -1)


def opposite(after, before, axis):
    half = after.shape[0] // 2
    return pull(after[:half], axis, 1), pull(before[half:], axis, -1)


def in_ring(value, near, far):
    return jnp.concatenate([value, near[0], *far, near[1]], axis=0)


def matmul(left, right):
    return jnp.dot(left, right, preferred_element_type=F32)


def matmul_t(left, right):
    return lax.dot_general(left, right, (((1,), (1,)), ((), ())), preferred_element_type=F32)


def rolled(value, axis, shift):
    return lax.dynamic_slice_in_dim(
        jnp.concatenate([value, value], axis=axis), shift, value.shape[axis], axis
    )


def norm_rows(values, gain):
    center = jnp.mean(values, axis=-1, keepdims=True)
    off = values - center
    spread = jnp.mean(off * off, axis=-1, keepdims=True)
    return (off * lax.rsqrt(spread + EPSILON) * gain).astype(BF16)


SIDES = (0, 1, 3, 2)


def across(value):
    blocks = [value] + [pull(value, "x", d) for d in (2, 1, 3)]
    near = jnp.concatenate([blocks[0], blocks[2], blocks[3]], axis=0)
    return near, blocks[1], pull(near, "c", 1), pull(blocks[1], "c", 1)


def summed_rows(rows_other, rows_own):
    came = pull(rows_other.astype(BF16), "c", 1)
    pair = rows_own + came.astype(F32)
    count = pair.shape[0] // 4
    pieces = [pair[count * d : count * (d + 1)] for d in range(4)]
    total = pieces[0]
    for d in (2, 1, 3):
        total = total + pull(pieces[(-d) % 4].astype(BF16), "x", d).astype(F32)
    return total


def by_owner(value, x, core):
    split = value.reshape(4, 2, -1, value.shape[-1])
    out = []
    for c in (1 - core, core):
        part = lax.dynamic_index_in_dim(split, c, 1, keepdims=False)
        out.append(rolled(part, 0, x).reshape(-1, value.shape[-1]))
    return out


def in_order(blocks, x, core):
    flat = jnp.stack(
        [
            jnp.stack([jnp.where(core == 0, a, b), jnp.where(core == 0, b, a)])
            for a, b in blocks
        ]
    )
    return rolled(flat, 0, (4 - x) % 4).reshape(-1, flat.shape[-1])


def channel_stats(mixed):
    count = mixed.shape[-1]
    mean = jnp.sum(mixed, axis=-1) / count
    off = mixed - mean[:, None]
    square = jnp.sum(off * off, axis=-1)
    both = jnp.concatenate([mean, square]).reshape(1, 1, -1)
    both = jnp.broadcast_to(both, (8, 1, both.shape[-1]))
    both = lax.all_to_all(both, "tp", split_axis=0, concat_axis=0, tiled=True)
    mean, square = both[:, 0, : mean.size], both[:, 0, mean.size :]
    center = jnp.mean(mean, axis=0)
    off = mean - center
    spread = jnp.mean(square, axis=0) / count + jnp.mean(off * off, axis=0)
    return center[:, None], spread[:, None]


def body(
    tokens,
    first_gate,
    first_up,
    first_down,
    first_gain,
    glu_value,
    glu_gate,
    conv_taps,
    conv_gain,
    conv_proj,
    second_gain,
    last_gate,
    last_up,
    last_down,
    third_gain,
):
    tp = lax.axis_index("tp")
    fs = lax.axis_index("fs")
    x, core = tp // 2, tp % 2
    z, y = fs // 4, fs % 4
    current = tokens[0]

    early = lax.all_gather(
        jnp.concatenate([first_down.T, glu_value, glu_gate, conv_proj.T], axis=1),
        "fs",
        axis=0,
        tiled=True,
    )
    late = lax.all_gather(
        jnp.concatenate([last_gate, last_up, last_down.T], axis=1), "fs", axis=0, tiled=True
    )

    near_gate, near_up = neighbours(first_gate, "z"), neighbours(first_up, "y")
    far_gate, far_up = opposite(*near_gate, "z"), opposite(*near_up, "y")
    gate_part = in_ring(first_gate, near_gate, far_gate)
    up_part = in_ring(first_up, near_up, far_up)

    length = current.shape[0]
    gains = jnp.stack([first_gain, second_gain, third_gain])
    rows = jnp.concatenate([current, jnp.pad(gains, ((0, 5), (0, 0)))], axis=0)
    rows, _, _ = lax.optimization_barrier((rows, gate_part, up_part))
    blocks = [rows] + [pull(rows, "x", d) for d in (1, 2, 3)]
    blocks = [jnp.concatenate([b, pull(b, "c", 1)], axis=1) for b in blocks]
    turned = [rolled(b[:length], 1, ((y + 2 * core) % 4) * 128) for b in blocks]
    turned = rolled(jnp.concatenate(turned, axis=1), 1, ((z - x) % 4) * 512)
    some = [
        jnp.concatenate(
            [lax.dynamic_slice_in_dim(b, 48 * tp, 48, 0), b[length : length + 8]], axis=0
        )
        for b in blocks
    ]
    some = [rolled(b, 1, core * 256) for b in some]
    some = rolled(jnp.concatenate(some, axis=1), 1, ((4 - x) % 4) * 512)
    own_rows, gains = some[:48].astype(F32), some[48:51].astype(F32)

    near_gate, near_up = neighbours(gate_part, "y"), neighbours(up_part, "z")
    near_gate, near_up, turned = lax.optimization_barrier((near_gate, near_up, turned))
    far_gate, far_up = opposite(*near_gate, "y"), opposite(*near_up, "z")
    gate_of = [
        jnp.concatenate([turned[:, 512 * k + 128 * d :][:, :128] for k in range(4)], axis=1)
        for d in range(4)
    ]
    up_of = [turned[:, 512 * d : 512 * (d + 1)] for d in range(4)]

    def split_sum(left, own, near, far):
        total = matmul(left[0], own)
        total = total + matmul(left[1], near[0])
        total = total + matmul(left[3], near[1])
        total = total + matmul(left[2][:, :256], far[0])
        return total + matmul(left[2][:, 256:], far[1])

    gate = split_sum(gate_of, gate_part, near_gate, far_gate)
    up = split_sum(up_of, up_part, near_up, far_up)
    hidden = (jax.nn.silu(gate) * up).astype(BF16)

    def down(rows_other, rows_own, weight):
        return summed_rows(matmul_t(rows_other, weight), matmul_t(rows_own, weight))

    branch = down(*by_owner(hidden, x, core), early[:, :768])
    first = norm_rows(ALPHA * own_rows + 0.5 * branch, gains[0])

    def every_row(rows):
        near, far, near_other, far_other = across(rows)
        return jnp.concatenate([near, far, near_other, far_other], axis=0)

    def by_distance(values):
        count = values.shape[0] // 8
        at = [values[count * k : count * (k + 1)] for k in range(8)]
        own = [at[SIDES.index(d)] for d in range(4)]
        other = [at[4 + SIDES.index(d)] for d in range(4)]
        return own, other

    def gated_linear(rows):
        both = matmul(rows, early[:, 768:1024])
        return both[:, :128] * jax.nn.sigmoid(both[:, 128:])

    gated = in_order(list(zip(*by_distance(gated_linear(every_row(first))))), x, core)
    reach = (conv_taps.shape[0] - 1) // 2
    padded = jnp.pad(gated, ((reach, reach), (0, 0)))
    taps = conv_taps.astype(F32)
    mixed = jnp.zeros_like(gated)
    for k in range(conv_taps.shape[0]):
        mixed = mixed + taps[k] * padded[k : k + length]
    center, spread = channel_stats(mixed)
    normed = (mixed - center) * lax.rsqrt(spread + EPSILON) * conv_gain.astype(F32)
    act = jax.nn.silu(normed).astype(BF16)
    branch = down(*by_owner(act, x, core), early[:, 1024:])
    second = norm_rows(ALPHA * first.astype(F32) + branch, gains[1])

    def gated_hidden(rows):
        return (
            jax.nn.silu(matmul(rows, late[:, :768])) * matmul(rows, late[:, 768:1536])
        ).astype(BF16)

    own, other = by_distance(gated_hidden(every_row(second)))
    branch = down(
        jnp.concatenate(other, axis=0), jnp.concatenate(own, axis=0), late[:, 1536:]
    )
    out = norm_rows(ALPHA * second.astype(F32) + 0.5 * branch, gains[2])
    out = out.reshape(-1, 8, 256).transpose(1, 0, 2)
    out = lax.all_to_all(out, "tp", split_axis=0, concat_axis=0, tiled=True)
    return out.reshape(1, -1, 256)


def solution(mesh):
    return jax.shard_map(
        body,
        mesh=mesh,
        in_specs=(
            P("fs", None, "tp"),
            P("fs", "tp"),
            P("fs", "tp"),
            P("tp", "fs"),
            P("tp"),
            P("fs", "tp"),
            P("fs", "tp"),
            P(None, "tp"),
            P("tp"),
            P("tp", "fs"),
            P("tp"),
            P("fs", "tp"),
            P("fs", "tp"),
            P("tp", "fs"),
            P("tp"),
        ),
        out_specs=P("fs", None, "tp"),
        check_vma=False,
    )
```

```python
import jax
import jax.numpy as jnp
from jax import lax
from jax.experimental import pallas as pl
from jax.experimental.pallas import tpu as pltpu
from jax.sharding import PartitionSpec as P


ALPHA = 2.0**0.25
EPSILON = 1e-05
F32 = jnp.float32
BF16 = jnp.bfloat16


def pull(value, axis, distance):
    if axis == "z":
        pairs = [(i, ((i // 4 - distance) % 4) * 4 + i % 4) for i in range(16)]
    elif axis == "y":
        pairs = [(i, (i // 4) * 4 + (i % 4 - distance) % 4) for i in range(16)]
    elif axis == "x":
        pairs = [(i, ((i // 2 - distance) % 4) * 2 + i % 2) for i in range(8)]
    else:
        pairs = [(i, i ^ 1) for i in range(8)]
    return lax.ppermute(value, "fs" if axis in "zy" else "tp", pairs)


def neighbours(value, axis):
    return pull(value, axis, 1), pull(value, axis, -1)


def opposite(after, before, axis):
    half = after.shape[0] // 2
    return pull(after[:half], axis, 1), pull(before[half:], axis, -1)


def in_ring(value, near, far):
    return jnp.concatenate([value, near[0], *far, near[1]], axis=0)


def matmul(left, right):
    return jnp.dot(left, right, preferred_element_type=F32)


def matmul_t(left, right):
    return lax.dot_general(left, right, (((1,), (1,)), ((), ())), preferred_element_type=F32)


def gated_hidden(rows, weights, width):
    block = 256
    count = width // block

    def kernel(rows_ref, gate_ref, up_ref, out_ref):
        gate = matmul(rows_ref[...], gate_ref[...])
        up = matmul(rows_ref[...], up_ref[...])
        out_ref[...] = (jax.nn.silu(gate) * up).astype(BF16)

    depth = weights.shape[0]
    return pl.pallas_call(
        kernel,
        grid=(count,),
        in_specs=[
            pl.BlockSpec(rows.shape, lambda j: (0, 0)),
            pl.BlockSpec((depth, block), lambda j: (0, j)),
            pl.BlockSpec((depth, block), lambda j: (0, count + j)),
        ],
        out_specs=pl.BlockSpec((rows.shape[0], block), lambda j: (0, j)),
        out_shape=jax.ShapeDtypeStruct((rows.shape[0], width), BF16),
        compiler_params=pltpu.CompilerParams(vmem_limit_bytes=24 * 2**20),
        name="gated_hidden",
    )(rows, weights, weights)


def rolled(value, axis, shift):
    return lax.dynamic_slice_in_dim(
        jnp.concatenate([value, value], axis=axis), shift, value.shape[axis], axis
    )


def norm_rows(values, gain):
    center = jnp.mean(values, axis=-1, keepdims=True)
    off = values - center
    spread = jnp.mean(off * off, axis=-1, keepdims=True)
    return (off * lax.rsqrt(spread + EPSILON) * gain).astype(BF16)


SIDES = (0, 1, 3, 2)


def across(value):
    blocks = [value] + [pull(value, "x", d) for d in (2, 1, 3)]
    near = jnp.concatenate([blocks[0], blocks[2], blocks[3]], axis=0)
    return near, blocks[1], pull(near, "c", 1), pull(blocks[1], "c", 1)


def summed_rows(rows_other, rows_own):
    came = pull(rows_other.astype(BF16), "c", 1)
    pair = rows_own + came.astype(F32)
    count = pair.shape[0] // 4
    pieces = [pair[count * d : count * (d + 1)] for d in range(4)]
    total = pieces[0]
    for d in (2, 1, 3):
        total = total + pull(pieces[(-d) % 4].astype(BF16), "x", d).astype(F32)
    return total


def by_owner(value, x, core):
    split = value.reshape(4, 2, -1, value.shape[-1])
    out = []
    for c in (1 - core, core):
        part = lax.dynamic_index_in_dim(split, c, 1, keepdims=False)
        out.append(rolled(part, 0, x).reshape(-1, value.shape[-1]))
    return out


def in_order(blocks, x, core):
    flat = jnp.stack(
        [
            jnp.stack([jnp.where(core == 0, a, b), jnp.where(core == 0, b, a)])
            for a, b in blocks
        ]
    )
    return rolled(flat, 0, (4 - x) % 4).reshape(-1, flat.shape[-1])


def channel_stats(mixed):
    count = mixed.shape[-1]
    mean = jnp.sum(mixed, axis=-1) / count
    off = mixed - mean[:, None]
    square = jnp.sum(off * off, axis=-1)
    both = jnp.concatenate([mean, square]).reshape(1, 1, -1)
    both = jnp.broadcast_to(both, (8, 1, both.shape[-1]))
    both = lax.all_to_all(both, "tp", split_axis=0, concat_axis=0, tiled=True)
    mean, square = both[:, 0, : mean.size], both[:, 0, mean.size :]
    center = jnp.mean(mean, axis=0)
    off = mean - center
    spread = jnp.mean(square, axis=0) / count + jnp.mean(off * off, axis=0)
    return center[:, None], spread[:, None]


def layer(
    tokens,
    first_gate,
    first_up,
    first_down,
    first_gain,
    glu_value,
    glu_gate,
    conv_taps,
    conv_gain,
    conv_proj,
    second_gain,
    last_gate,
    last_up,
    last_down,
    third_gain,
):
    tp = lax.axis_index("tp")
    fs = lax.axis_index("fs")
    x, core = tp // 2, tp % 2
    z, y = fs // 4, fs % 4
    current = tokens[0]

    early = lax.all_gather(
        jnp.concatenate([first_down.T, glu_value, glu_gate, conv_proj.T], axis=1),
        "fs",
        axis=0,
        tiled=True,
    )

    near_gate, near_up = neighbours(first_gate, "z"), neighbours(first_up, "y")
    far_gate, far_up = opposite(*near_gate, "z"), opposite(*near_up, "y")
    gate_part = in_ring(first_gate, near_gate, far_gate)
    up_part = in_ring(first_up, near_up, far_up)

    arrays = (last_gate, last_up, last_down, current, first_gain, second_gain, third_gain)
    (*last, current, g1, g2, g3), _, _ = lax.optimization_barrier((arrays, gate_part, up_part))
    last = jnp.concatenate([last[0], last[1], last[2].T], axis=1)
    (current, g1, g2, g3), last = lax.optimization_barrier(((current, g1, g2, g3), last))
    late = lax.all_gather(last, "fs", axis=0, tiled=True)

    length = current.shape[0]
    gains = jnp.pad(jnp.stack([g1, g2, g3]), ((0, 5), (0, 0)))
    rows = jnp.concatenate([current, gains], axis=0)
    blocks = [rows] + [pull(rows, "x", d) for d in (1, 2, 3)]
    blocks = [jnp.concatenate([b, pull(b, "c", 1)], axis=1) for b in blocks]
    turned = [rolled(b[:length], 1, ((y + 2 * core) % 4) * 128) for b in blocks]
    turned = rolled(jnp.concatenate(turned, axis=1), 1, ((z - x) % 4) * 512)
    some = [
        jnp.concatenate(
            [lax.dynamic_slice_in_dim(b, 48 * tp, 48, 0), b[length : length + 8]], axis=0
        )
        for b in blocks
    ]
    some = [rolled(b, 1, core * 256) for b in some]
    some = rolled(jnp.concatenate(some, axis=1), 1, ((4 - x) % 4) * 512)
    own_rows, gains = some[:48].astype(F32), some[48:51].astype(F32)

    near_gate, near_up = neighbours(gate_part, "y"), neighbours(up_part, "z")
    near_gate, near_up, turned = lax.optimization_barrier((near_gate, near_up, turned))
    far_gate, far_up = opposite(*near_gate, "y"), opposite(*near_up, "z")
    gate_of = [
        jnp.concatenate([turned[:, 512 * k + 128 * d :][:, :128] for k in range(4)], axis=1)
        for d in range(4)
    ]
    up_of = [turned[:, 512 * d : 512 * (d + 1)] for d in range(4)]

    def split_sum(left, own, near, far):
        total = matmul(left[0], own)
        total = total + matmul(left[1], near[0])
        total = total + matmul(left[3], near[1])
        total = total + matmul(left[2][:, :256], far[0])
        return total + matmul(left[2][:, 256:], far[1])

    gate = split_sum(gate_of, gate_part, near_gate, far_gate)
    up = split_sum(up_of, up_part, near_up, far_up)
    hidden = (jax.nn.silu(gate) * up).astype(BF16)

    def down(rows_other, rows_own, weight):
        return summed_rows(matmul_t(rows_other, weight), matmul_t(rows_own, weight))

    branch = down(*by_owner(hidden, x, core), early[:, :768])
    first = norm_rows(ALPHA * own_rows + 0.5 * branch, gains[0])

    def every_row(rows):
        near, far, near_other, far_other = across(rows)
        return jnp.concatenate([near, far, near_other, far_other], axis=0)

    def by_distance(values):
        count = values.shape[0] // 8
        at = [values[count * k : count * (k + 1)] for k in range(8)]
        own = [at[SIDES.index(d)] for d in range(4)]
        other = [at[4 + SIDES.index(d)] for d in range(4)]
        return own, other

    def gated_linear(rows):
        both = matmul(rows, early[:, 768:1024])
        return both[:, :128] * jax.nn.sigmoid(both[:, 128:])

    gated = in_order(list(zip(*by_distance(gated_linear(every_row(first))))), x, core)
    reach = (conv_taps.shape[0] - 1) // 2
    padded = jnp.pad(gated, ((reach, reach), (0, 0)))
    taps = conv_taps.astype(F32)
    mixed = jnp.zeros_like(gated)
    for k in range(conv_taps.shape[0]):
        mixed = mixed + taps[k] * padded[k : k + length]
    center, spread = channel_stats(mixed)
    normed = (mixed - center) * lax.rsqrt(spread + EPSILON) * conv_gain.astype(F32)
    act = jax.nn.silu(normed).astype(BF16)
    branch = down(*by_owner(act, x, core), early[:, 1024:])
    second = norm_rows(ALPHA * first.astype(F32) + branch, gains[1])

    own, other = by_distance(gated_hidden(every_row(second), late, 768))
    branch = down(
        jnp.concatenate(other, axis=0), jnp.concatenate(own, axis=0), late[:, 1536:]
    )
    out = norm_rows(ALPHA * second.astype(F32) + 0.5 * branch, gains[2])
    out = out.reshape(-1, 8, 256).transpose(1, 0, 2)
    out = lax.all_to_all(out, "tp", split_axis=0, concat_axis=0, tiled=True)
    return out.reshape(1, -1, 256)


def solution(mesh):
    return jax.shard_map(
        layer,
        mesh=mesh,
        in_specs=(
            P("fs", None, "tp"),
            P("fs", "tp"),
            P("fs", "tp"),
            P("tp", "fs"),
            P("tp"),
            P("fs", "tp"),
            P("fs", "tp"),
            P(None, "tp"),
            P("tp"),
            P("tp", "fs"),
            P("tp"),
            P("fs", "tp"),
            P("fs", "tp"),
            P("tp", "fs"),
            P("tp"),
        ),
        out_specs=P("fs", None, "tp"),
        check_vma=False,
    )
```

```python
import jax
import jax.numpy as jnp
from jax import lax
from jax.experimental import pallas as pl
from jax.experimental.pallas import tpu as pltpu
from jax.sharding import PartitionSpec as P


ALPHA = 2.0**0.25
EPSILON = 1e-05
F32 = jnp.float32
BF16 = jnp.bfloat16


def pull(value, axis, distance):
    if axis == "z":
        pairs = [(i, ((i // 4 - distance) % 4) * 4 + i % 4) for i in range(16)]
    elif axis == "y":
        pairs = [(i, (i // 4) * 4 + (i % 4 - distance) % 4) for i in range(16)]
    elif axis == "x":
        pairs = [(i, ((i // 2 - distance) % 4) * 2 + i % 2) for i in range(8)]
    else:
        pairs = [(i, i ^ 1) for i in range(8)]
    return lax.ppermute(value, "fs" if axis in "zy" else "tp", pairs)


def neighbours(value, axis):
    return pull(value, axis, 1), pull(value, axis, -1)


def opposite(after, before, axis):
    half = after.shape[0] // 2
    return pull(after[:half], axis, 1), pull(before[half:], axis, -1)


def in_ring(value, near, far):
    return jnp.concatenate([value, near[0], *far, near[1]], axis=0)


def matmul(left, right):
    return jnp.dot(left, right, preferred_element_type=F32)


def matmul_t(left, right):
    return lax.dot_general(left, right, (((1,), (1,)), ((), ())), preferred_element_type=F32)


def gated_hidden(rows, weights, width):
    block = 256
    count = width // block

    def kernel(rows_ref, gate_ref, up_ref, out_ref):
        gate = matmul(rows_ref[...], gate_ref[...])
        up = matmul(rows_ref[...], up_ref[...])
        out_ref[...] = (jax.nn.silu(gate) * up).astype(BF16)

    depth = weights.shape[0]
    return pl.pallas_call(
        kernel,
        grid=(count,),
        in_specs=[
            pl.BlockSpec(rows.shape, lambda j: (0, 0)),
            pl.BlockSpec((depth, block), lambda j: (0, j)),
            pl.BlockSpec((depth, block), lambda j: (0, count + j)),
        ],
        out_specs=pl.BlockSpec((rows.shape[0], block), lambda j: (0, j)),
        out_shape=jax.ShapeDtypeStruct((rows.shape[0], width), BF16),
        compiler_params=pltpu.CompilerParams(vmem_limit_bytes=24 * 2**20),
        name="gated_hidden",
    )(rows, weights, weights)


def rolled(value, axis, shift):
    return lax.dynamic_slice_in_dim(
        jnp.concatenate([value, value], axis=axis), shift, value.shape[axis], axis
    )


def norm_rows(values, gain):
    center = jnp.mean(values, axis=-1, keepdims=True)
    off = values - center
    spread = jnp.mean(off * off, axis=-1, keepdims=True)
    return (off * lax.rsqrt(spread + EPSILON) * gain).astype(BF16)


SIDES = (0, 1, 3, 2)


def across(value):
    blocks = [value] + [pull(value, "x", d) for d in (2, 1, 3)]
    near = jnp.concatenate([blocks[0], blocks[2], blocks[3]], axis=0)
    near_other = pull(near, "c", 1)
    return near, blocks[1], near_other, pull(blocks[1], "c", 1)


def summed_rows(rows_other, rows_own):
    rows_own = lax.optimization_barrier(rows_own)
    came = pull(rows_other.astype(BF16), "c", 1)
    pair = rows_own + came.astype(F32)
    count = pair.shape[0] // 4
    pieces = [pair[count * d : count * (d + 1)] for d in range(4)]
    total = pieces[0]
    for d in (2, 1, 3):
        total = total + pull(pieces[(-d) % 4].astype(BF16), "x", d).astype(F32)
    return total


def by_owner(value, x, core):
    split = value.reshape(4, 2, -1, value.shape[-1])
    out = []
    for c in (1 - core, core):
        part = lax.dynamic_index_in_dim(split, c, 1, keepdims=False)
        out.append(rolled(part, 0, x).reshape(-1, value.shape[-1]))
    return out


def in_order(blocks, x, core):
    flat = jnp.stack(
        [
            jnp.stack([jnp.where(core == 0, a, b), jnp.where(core == 0, b, a)])
            for a, b in blocks
        ]
    )
    return rolled(flat, 0, (4 - x) % 4).reshape(-1, flat.shape[-1])


def channel_stats(mixed):
    count = mixed.shape[-1]
    mean = jnp.sum(mixed, axis=-1) / count
    off = mixed - mean[:, None]
    square = jnp.sum(off * off, axis=-1)
    both = jnp.concatenate([mean, square]).reshape(1, 1, -1)
    both = jnp.broadcast_to(both, (8, 1, both.shape[-1]))
    both = lax.all_to_all(both, "tp", split_axis=0, concat_axis=0, tiled=True)
    mean, square = both[:, 0, : mean.size], both[:, 0, mean.size :]
    center = jnp.mean(mean, axis=0)
    off = mean - center
    spread = jnp.mean(square, axis=0) / count + jnp.mean(off * off, axis=0)
    return center[:, None], spread[:, None]


def layer(
    tokens,
    first_gate,
    first_up,
    first_down,
    first_gain,
    glu_value,
    glu_gate,
    conv_taps,
    conv_gain,
    conv_proj,
    second_gain,
    last_gate,
    last_up,
    last_down,
    third_gain,
):
    tp = lax.axis_index("tp")
    fs = lax.axis_index("fs")
    x, core = tp // 2, tp % 2
    z, y = fs // 4, fs % 4
    current = tokens[0]

    early = lax.all_gather(
        jnp.concatenate([first_down.T, glu_value, glu_gate, conv_proj.T], axis=1),
        "fs",
        axis=0,
        tiled=True,
    )

    near_gate, near_up = neighbours(first_gate, "z"), neighbours(first_up, "y")
    far_gate, far_up = opposite(*near_gate, "z"), opposite(*near_up, "y")
    gate_part = in_ring(first_gate, near_gate, far_gate)
    up_part = in_ring(first_up, near_up, far_up)

    arrays = (last_gate, last_up, last_down, current, first_gain, second_gain, third_gain)
    (*last, current, g1, g2, g3), _, _ = lax.optimization_barrier((arrays, gate_part, up_part))
    last = jnp.concatenate([last[0], last[1], last[2].T], axis=1)
    (current, g1, g2, g3), last = lax.optimization_barrier(((current, g1, g2, g3), last))
    late = lax.all_gather(last, "fs", axis=0, tiled=True)

    length = current.shape[0]
    gains = jnp.pad(jnp.stack([g1, g2, g3]), ((0, 5), (0, 0)))
    rows = jnp.concatenate([current, gains], axis=0)
    blocks = [rows] + [pull(rows, "x", d) for d in (1, 2, 3)]
    blocks = [jnp.concatenate([b, pull(b, "c", 1)], axis=1) for b in blocks]
    turned = [rolled(b[:length], 1, ((y + 2 * core) % 4) * 128) for b in blocks]
    turned = rolled(jnp.concatenate(turned, axis=1), 1, ((z - x) % 4) * 512)
    some = [
        jnp.concatenate(
            [lax.dynamic_slice_in_dim(b, 48 * tp, 48, 0), b[length : length + 8]], axis=0
        )
        for b in blocks
    ]
    some = [rolled(b, 1, core * 256) for b in some]
    some = rolled(jnp.concatenate(some, axis=1), 1, ((4 - x) % 4) * 512)
    own_rows, gains = some[:48].astype(F32), some[48:51].astype(F32)

    near_gate, near_up = neighbours(gate_part, "y"), neighbours(up_part, "z")
    near_gate, near_up, turned = lax.optimization_barrier((near_gate, near_up, turned))
    far_gate, far_up = opposite(*near_gate, "y"), opposite(*near_up, "z")
    gate_of = [
        jnp.concatenate([turned[:, 512 * k + 128 * d :][:, :128] for k in range(4)], axis=1)
        for d in range(4)
    ]
    up_of = [turned[:, 512 * d : 512 * (d + 1)] for d in range(4)]

    def split_sum(left, own, near, far):
        total = matmul(left[0], own)
        total = total + matmul(left[1], near[0])
        total = total + matmul(left[3], near[1])
        total = total + matmul(left[2][:, :256], far[0])
        return total + matmul(left[2][:, 256:], far[1])

    gate = split_sum(gate_of, gate_part, near_gate, far_gate)
    up = split_sum(up_of, up_part, near_up, far_up)
    hidden = (jax.nn.silu(gate) * up).astype(BF16)

    def down(rows_other, rows_own, weight):
        return summed_rows(matmul_t(rows_other, weight), matmul_t(rows_own, weight))

    branch = down(*by_owner(hidden, x, core), early[:, :768])
    first = norm_rows(ALPHA * own_rows + 0.5 * branch, gains[0])

    def every_row(rows):
        near, far, near_other, far_other = across(rows)
        return jnp.concatenate([near, far, near_other, far_other], axis=0)

    def by_distance(values):
        count = values.shape[0] // 8
        at = [values[count * k : count * (k + 1)] for k in range(8)]
        own = [at[SIDES.index(d)] for d in range(4)]
        other = [at[4 + SIDES.index(d)] for d in range(4)]
        return own, other

    def gated_linear(rows):
        both = matmul(rows, early[:, 768:1024])
        return both[:, :128] * jax.nn.sigmoid(both[:, 128:])

    gated = in_order(list(zip(*by_distance(gated_linear(every_row(first))))), x, core)
    reach = (conv_taps.shape[0] - 1) // 2
    padded = jnp.pad(gated, ((reach, reach), (0, 0)))
    taps = conv_taps.astype(F32)
    mixed = jnp.zeros_like(gated)
    for k in range(conv_taps.shape[0]):
        mixed = mixed + taps[k] * padded[k : k + length]
    center, spread = channel_stats(mixed)
    normed = (mixed - center) * lax.rsqrt(spread + EPSILON) * conv_gain.astype(F32)
    act = jax.nn.silu(normed).astype(BF16)
    branch = down(*by_owner(act, x, core), early[:, 1024:])
    second = norm_rows(ALPHA * first.astype(F32) + branch, gains[1])

    rows = every_row(second)
    own, other = by_distance(gated_hidden(rows, late, 768))
    branch = down(
        jnp.concatenate(other, axis=0), jnp.concatenate(own, axis=0), late[:, 1536:]
    )
    out = norm_rows(ALPHA * second.astype(F32) + 0.5 * branch, gains[2])
    out = out.reshape(-1, 8, 256).transpose(1, 0, 2)
    out = lax.all_to_all(out, "tp", split_axis=0, concat_axis=0, tiled=True)
    return out.reshape(1, -1, 256)


def solution(mesh):
    return jax.shard_map(
        layer,
        mesh=mesh,
        in_specs=(
            P("fs", None, "tp"),
            P("fs", "tp"),
            P("fs", "tp"),
            P("tp", "fs"),
            P("tp"),
            P("fs", "tp"),
            P("fs", "tp"),
            P(None, "tp"),
            P("tp"),
            P("tp", "fs"),
            P("tp"),
            P("fs", "tp"),
            P("fs", "tp"),
            P("tp", "fs"),
            P("tp"),
        ),
        out_specs=P("fs", None, "tp"),
        check_vma=False,
    )
```

```python
import jax
import jax.numpy as jnp
from jax import lax
from jax.experimental import pallas as pl
from jax.experimental.pallas import tpu as pltpu
from jax.sharding import PartitionSpec as P


ALPHA = 2.0**0.25
EPSILON = 1e-05
F32 = jnp.float32
BF16 = jnp.bfloat16


def pull(value, axis, distance):
    if axis == "z":
        pairs = [(i, ((i // 4 - distance) % 4) * 4 + i % 4) for i in range(16)]
    elif axis == "y":
        pairs = [(i, (i // 4) * 4 + (i % 4 - distance) % 4) for i in range(16)]
    elif axis == "x":
        pairs = [(i, ((i // 2 - distance) % 4) * 2 + i % 2) for i in range(8)]
    else:
        pairs = [(i, i ^ 1) for i in range(8)]
    return lax.ppermute(value, "fs" if axis in "zy" else "tp", pairs)


def neighbours(value, axis):
    return pull(value, axis, 1), pull(value, axis, -1)


def opposite(after, before, axis):
    half = after.shape[0] // 2
    return pull(after[:half], axis, 1), pull(before[half:], axis, -1)


def in_ring(value, near, far):
    return jnp.concatenate([value, near[0], *far, near[1]], axis=0)


def matmul(left, right):
    return jnp.dot(left, right, preferred_element_type=F32)


def matmul_t(left, right):
    return lax.dot_general(left, right, (((1,), (1,)), ((), ())), preferred_element_type=F32)


def packed(down, proj, value, gate):
    sizes = [down.shape[0], proj.shape[0], value.shape[1], gate.shape[1]]
    ends = [sum(sizes[: k + 1]) for k in range(4)]

    def kernel(down_ref, proj_ref, value_ref, gate_ref, out_ref):
        out_ref[: ends[0]] = down_ref[...]
        out_ref[ends[0] : ends[1]] = proj_ref[...]
        out_ref[ends[1] : ends[2]] = value_ref[...].T
        out_ref[ends[2] :] = gate_ref[...].T

    return pl.pallas_call(
        kernel,
        out_shape=jax.ShapeDtypeStruct((ends[3], down.shape[1]), BF16),
        name="packed",
    )(down, proj, value, gate)


def gated_hidden(rows, weights, width):
    block = 256
    count = width // block

    def kernel(rows_ref, gate_ref, up_ref, out_ref):
        gate = matmul(rows_ref[...], gate_ref[...])
        up = matmul(rows_ref[...], up_ref[...])
        out_ref[...] = (jax.nn.silu(gate) * up).astype(BF16)

    depth = weights.shape[0]
    return pl.pallas_call(
        kernel,
        grid=(count,),
        in_specs=[
            pl.BlockSpec(rows.shape, lambda j: (0, 0)),
            pl.BlockSpec((depth, block), lambda j: (0, j)),
            pl.BlockSpec((depth, block), lambda j: (0, count + j)),
        ],
        out_specs=pl.BlockSpec((rows.shape[0], block), lambda j: (0, j)),
        out_shape=jax.ShapeDtypeStruct((rows.shape[0], width), BF16),
        compiler_params=pltpu.CompilerParams(vmem_limit_bytes=24 * 2**20),
        name="gated_hidden",
    )(rows, weights, weights)


def rolled(value, axis, shift):
    return lax.dynamic_slice_in_dim(
        jnp.concatenate([value, value], axis=axis), shift, value.shape[axis], axis
    )


def norm_rows(values, gain):
    center = jnp.mean(values, axis=-1, keepdims=True)
    off = values - center
    spread = jnp.mean(off * off, axis=-1, keepdims=True)
    return (off * lax.rsqrt(spread + EPSILON) * gain).astype(BF16)


SIDES = (0, 1, 3, 2)


def across(value):
    blocks = [value] + [pull(value, "x", d) for d in (2, 1, 3)]
    near = jnp.concatenate([blocks[0], blocks[2], blocks[3]], axis=0)
    near_other = pull(near, "c", 1)
    return near, blocks[1], near_other, pull(blocks[1], "c", 1)


def summed_rows(rows_other, rows_own):
    rows_own = lax.optimization_barrier(rows_own)
    came = pull(rows_other.astype(BF16), "c", 1)
    pair = rows_own + came.astype(F32)
    count = pair.shape[0] // 4
    pieces = [pair[count * d : count * (d + 1)] for d in range(4)]
    total = pieces[0]
    for d in (2, 1, 3):
        total = total + pull(pieces[(-d) % 4].astype(BF16), "x", d).astype(F32)
    return total


def by_owner(value, x, core):
    split = value.reshape(4, 2, -1, value.shape[-1])
    out = []
    for c in (1 - core, core):
        part = lax.dynamic_index_in_dim(split, c, 1, keepdims=False)
        out.append(rolled(part, 0, x).reshape(-1, value.shape[-1]))
    return out


def in_order(blocks, x, core):
    flat = jnp.stack(
        [
            jnp.stack([jnp.where(core == 0, a, b), jnp.where(core == 0, b, a)])
            for a, b in blocks
        ]
    )
    return rolled(flat, 0, (4 - x) % 4).reshape(-1, flat.shape[-1])


def channel_stats(mixed):
    count = mixed.shape[-1]
    mean = jnp.sum(mixed, axis=-1) / count
    off = mixed - mean[:, None]
    square = jnp.sum(off * off, axis=-1)
    both = jnp.concatenate([mean, square]).reshape(1, 1, -1)
    both = jnp.broadcast_to(both, (8, 1, both.shape[-1]))
    both = lax.all_to_all(both, "tp", split_axis=0, concat_axis=0, tiled=True)
    mean, square = both[:, 0, : mean.size], both[:, 0, mean.size :]
    center = jnp.mean(mean, axis=0)
    off = mean - center
    spread = jnp.mean(square, axis=0) / count + jnp.mean(off * off, axis=0)
    return center[:, None], spread[:, None]


def layer(
    tokens,
    first_gate,
    first_up,
    first_down,
    first_gain,
    glu_value,
    glu_gate,
    conv_taps,
    conv_gain,
    conv_proj,
    second_gain,
    last_gate,
    last_up,
    last_down,
    third_gain,
):
    tp = lax.axis_index("tp")
    fs = lax.axis_index("fs")
    x, core = tp // 2, tp % 2
    z, y = fs // 4, fs % 4
    current = tokens[0]

    early = lax.all_gather(
        packed(first_down, conv_proj, glu_value, glu_gate), "fs", axis=1, tiled=True
    )

    near_gate, near_up = neighbours(first_gate, "z"), neighbours(first_up, "y")
    far_gate, far_up = opposite(*near_gate, "z"), opposite(*near_up, "y")
    gate_part = in_ring(first_gate, near_gate, far_gate)
    up_part = in_ring(first_up, near_up, far_up)

    arrays = (last_gate, last_up, last_down, current, first_gain, second_gain, third_gain)
    (*last, current, g1, g2, g3), _, _ = lax.optimization_barrier((arrays, gate_part, up_part))
    last = jnp.concatenate([last[0], last[1], last[2].T], axis=1)
    (current, g1, g2, g3), last = lax.optimization_barrier(((current, g1, g2, g3), last))
    late = lax.all_gather(last, "fs", axis=0, tiled=True)

    length = current.shape[0]
    gains = jnp.pad(jnp.stack([g1, g2, g3]), ((0, 5), (0, 0)))
    rows = jnp.concatenate([current, gains], axis=0)
    blocks = [rows] + [pull(rows, "x", d) for d in (1, 2, 3)]
    blocks = [jnp.concatenate([b, pull(b, "c", 1)], axis=1) for b in blocks]
    turned = [rolled(b[:length], 1, ((y + 2 * core) % 4) * 128) for b in blocks]
    turned = rolled(jnp.concatenate(turned, axis=1), 1, ((z - x) % 4) * 512)
    some = [
        jnp.concatenate(
            [lax.dynamic_slice_in_dim(b, 48 * tp, 48, 0), b[length : length + 8]], axis=0
        )
        for b in blocks
    ]
    some = [rolled(b, 1, core * 256) for b in some]
    some = rolled(jnp.concatenate(some, axis=1), 1, ((4 - x) % 4) * 512)
    own_rows, gains = some[:48].astype(F32), some[48:51].astype(F32)

    near_gate, near_up = neighbours(gate_part, "y"), neighbours(up_part, "z")
    far_gate, far_up = opposite(*near_gate, "y"), opposite(*near_up, "z")
    gate_of = [
        jnp.concatenate([turned[:, 512 * k + 128 * d :][:, :128] for k in range(4)], axis=1)
        for d in range(4)
    ]
    up_of = [turned[:, 512 * d : 512 * (d + 1)] for d in range(4)]

    def split_sum(left, own, near, far):
        total = matmul(left[0], own)
        total = total + matmul(left[1], near[0])
        total = total + matmul(left[3], near[1])
        total = total + matmul(left[2][:, :256], far[0])
        return total + matmul(left[2][:, 256:], far[1])

    gate = split_sum(gate_of, gate_part, near_gate, far_gate)
    up = split_sum(up_of, up_part, near_up, far_up)
    hidden = (jax.nn.silu(gate) * up).astype(BF16)

    def down(rows_other, rows_own, weight, product=matmul):
        return summed_rows(product(rows_other, weight), product(rows_own, weight))

    branch = down(*by_owner(hidden, x, core), early[:768])
    first = norm_rows(ALPHA * own_rows + 0.5 * branch, gains[0])

    def every_row(rows):
        near, far, near_other, far_other = across(rows)
        return jnp.concatenate([near, far, near_other, far_other], axis=0)

    def by_distance(values):
        count = values.shape[0] // 8
        at = [values[count * k : count * (k + 1)] for k in range(8)]
        own = [at[SIDES.index(d)] for d in range(4)]
        other = [at[4 + SIDES.index(d)] for d in range(4)]
        return own, other

    def gated_linear(rows):
        both = matmul_t(rows, early[896:])
        return both[:, :128] * jax.nn.sigmoid(both[:, 128:])

    gated = in_order(list(zip(*by_distance(gated_linear(every_row(first))))), x, core)
    reach = (conv_taps.shape[0] - 1) // 2
    padded = jnp.pad(gated, ((reach, reach), (0, 0)))
    taps = conv_taps.astype(F32)
    mixed = jnp.zeros_like(gated)
    for k in range(conv_taps.shape[0]):
        mixed = mixed + taps[k] * padded[k : k + length]
    center, spread = channel_stats(mixed)
    normed = (mixed - center) * lax.rsqrt(spread + EPSILON) * conv_gain.astype(F32)
    act = jax.nn.silu(normed).astype(BF16)
    branch = down(*by_owner(act, x, core), early[768:896])
    second = norm_rows(ALPHA * first.astype(F32) + branch, gains[1])

    rows = every_row(second)
    own, other = by_distance(gated_hidden(rows, late, 768))
    branch = down(
        jnp.concatenate(other, axis=0), jnp.concatenate(own, axis=0), late[:, 1536:], matmul_t
    )
    out = norm_rows(ALPHA * second.astype(F32) + 0.5 * branch, gains[2])
    out = out.reshape(-1, 8, 256).transpose(1, 0, 2)
    out = lax.all_to_all(out, "tp", split_axis=0, concat_axis=0, tiled=True)
    return out.reshape(1, -1, 256)


def solution(mesh):
    return jax.shard_map(
        layer,
        mesh=mesh,
        in_specs=(
            P("fs", None, "tp"),
            P("fs", "tp"),
            P("fs", "tp"),
            P("tp", "fs"),
            P("tp"),
            P("fs", "tp"),
            P("fs", "tp"),
            P(None, "tp"),
            P("tp"),
            P("tp", "fs"),
            P("tp"),
            P("fs", "tp"),
            P("fs", "tp"),
            P("tp", "fs"),
            P("tp"),
        ),
        out_specs=P("fs", None, "tp"),
        check_vma=False,
    )
```

```python
import jax
import jax.numpy as jnp
from jax import lax
from jax.experimental import pallas as pl
from jax.experimental.pallas import tpu as pltpu
from jax.sharding import PartitionSpec as P


ALPHA = 2.0**0.25
EPSILON = 1e-05
F32 = jnp.float32
BF16 = jnp.bfloat16


def pull(value, axis, distance):
    if axis == "z":
        pairs = [(i, ((i // 4 - distance) % 4) * 4 + i % 4) for i in range(16)]
    elif axis == "y":
        pairs = [(i, (i // 4) * 4 + (i % 4 - distance) % 4) for i in range(16)]
    elif axis == "x":
        pairs = [(i, ((i // 2 - distance) % 4) * 2 + i % 2) for i in range(8)]
    else:
        pairs = [(i, i ^ 1) for i in range(8)]
    return lax.ppermute(value, "fs" if axis in "zy" else "tp", pairs)


def neighbours(value, axis):
    return pull(value, axis, 1), pull(value, axis, -1)


def opposite(after, before, axis):
    half = after.shape[0] // 2
    return pull(after[:half], axis, 1), pull(before[half:], axis, -1)


def in_ring(value, near, far):
    return jnp.concatenate([value, near[0], *far, near[1]], axis=0)


def matmul(left, right):
    return jnp.dot(left, right, preferred_element_type=F32)


def matmul_t(left, right):
    return lax.dot_general(left, right, (((1,), (1,)), ((), ())), preferred_element_type=F32)


def packed(down, proj, value, gate):
    sizes = [down.shape[0], proj.shape[0], value.shape[1], gate.shape[1]]
    ends = [sum(sizes[: k + 1]) for k in range(4)]

    def kernel(down_ref, proj_ref, value_ref, gate_ref, out_ref):
        out_ref[: ends[0]] = down_ref[...]
        out_ref[ends[0] : ends[1]] = proj_ref[...]
        out_ref[ends[1] : ends[2]] = value_ref[...].T
        out_ref[ends[2] :] = gate_ref[...].T

    return pl.pallas_call(
        kernel,
        out_shape=jax.ShapeDtypeStruct((ends[3], down.shape[1]), BF16),
        name="packed",
    )(down, proj, value, gate)


def gated_hidden(rows, weights, width):
    block = 256
    count = width // block

    def kernel(rows_ref, gate_ref, up_ref, out_ref):
        gate = matmul(rows_ref[...], gate_ref[...])
        up = matmul(rows_ref[...], up_ref[...])
        out_ref[...] = (jax.nn.silu(gate) * up).astype(BF16)

    depth = weights.shape[0]
    source = pltpu.with_memory_space_constraint(weights, pltpu.HBM)
    return pl.pallas_call(
        kernel,
        grid=(count,),
        in_specs=[
            pl.BlockSpec(rows.shape, lambda j: (0, 0)),
            pl.BlockSpec((depth, block), lambda j: (0, j)),
            pl.BlockSpec((depth, block), lambda j: (0, count + j)),
        ],
        out_specs=pl.BlockSpec((rows.shape[0], block), lambda j: (0, j)),
        out_shape=jax.ShapeDtypeStruct((rows.shape[0], width), BF16),
        compiler_params=pltpu.CompilerParams(vmem_limit_bytes=24 * 2**20),
        name="gated_hidden",
    )(rows, source, source)


def rolled(value, axis, shift):
    return lax.dynamic_slice_in_dim(
        jnp.concatenate([value, value], axis=axis), shift, value.shape[axis], axis
    )


def norm_rows(values, gain):
    center = jnp.mean(values, axis=-1, keepdims=True)
    off = values - center
    spread = jnp.mean(off * off, axis=-1, keepdims=True)
    return (off * lax.rsqrt(spread + EPSILON) * gain).astype(BF16)


SIDES = (0, 1, 3, 2)


def across(value):
    blocks = [value] + [pull(value, "x", d) for d in (2, 1, 3)]
    near = jnp.concatenate([blocks[0], blocks[2], blocks[3]], axis=0)
    near_other = pull(near, "c", 1)
    far_other = pull(blocks[1], "c", 1)
    return near, blocks[1], near_other, far_other


def summed_rows(rows_other, rows_own):
    rows_own = lax.optimization_barrier(rows_own)
    came = pull(rows_other.astype(BF16), "c", 1)
    pair = rows_own + came.astype(F32)
    count = pair.shape[0] // 4
    pieces = [pair[count * d : count * (d + 1)] for d in range(4)]
    total = pieces[0]
    for d in (2, 1, 3):
        total = total + pull(pieces[(-d) % 4].astype(BF16), "x", d).astype(F32)
    return total


def by_owner(value, x, core):
    split = value.reshape(4, 2, -1, value.shape[-1])
    out = []
    for c in (1 - core, core):
        part = lax.dynamic_index_in_dim(split, c, 1, keepdims=False)
        out.append(rolled(part, 0, x).reshape(-1, value.shape[-1]))
    return out


def in_order(blocks, x, core):
    flat = jnp.stack(
        [
            jnp.stack([jnp.where(core == 0, a, b), jnp.where(core == 0, b, a)])
            for a, b in blocks
        ]
    )
    return rolled(flat, 0, (4 - x) % 4).reshape(-1, flat.shape[-1])


def channel_stats(mixed):
    count = mixed.shape[-1]
    mean = jnp.sum(mixed, axis=-1) / count
    off = mixed - mean[:, None]
    square = jnp.sum(off * off, axis=-1)
    both = jnp.concatenate([mean, square]).reshape(1, 1, -1)
    both = jnp.broadcast_to(both, (8, 1, both.shape[-1]))
    both = lax.all_to_all(both, "tp", split_axis=0, concat_axis=0, tiled=True)
    mean, square = both[:, 0, : mean.size], both[:, 0, mean.size :]
    center = jnp.mean(mean, axis=0)
    off = mean - center
    spread = jnp.mean(square, axis=0) / count + jnp.mean(off * off, axis=0)
    return center[:, None], spread[:, None]


def layer(
    tokens,
    first_gate,
    first_up,
    first_down,
    first_gain,
    glu_value,
    glu_gate,
    conv_taps,
    conv_gain,
    conv_proj,
    second_gain,
    last_gate,
    last_up,
    last_down,
    third_gain,
):
    tp = lax.axis_index("tp")
    fs = lax.axis_index("fs")
    x, core = tp // 2, tp % 2
    z, y = fs // 4, fs % 4
    current = tokens[0]

    early = lax.all_gather(
        packed(first_down, conv_proj, glu_value, glu_gate), "fs", axis=1, tiled=True
    )

    near_gate, near_up = neighbours(first_gate, "z"), neighbours(first_up, "y")
    far_gate, far_up = opposite(*near_gate, "z"), opposite(*near_up, "y")
    gate_part = in_ring(first_gate, near_gate, far_gate)
    up_part = in_ring(first_up, near_up, far_up)

    arrays = (last_gate, last_up, last_down, current, first_gain, second_gain, third_gain)
    (*last, current, g1, g2, g3), _, _ = lax.optimization_barrier((arrays, gate_part, up_part))
    last = jnp.concatenate([last[0], last[1], last[2].T], axis=1)
    (current, g1, g2, g3), last = lax.optimization_barrier(((current, g1, g2, g3), last))
    late = lax.all_gather(last, "fs", axis=0, tiled=True)

    length = current.shape[0]
    gains = jnp.pad(jnp.stack([g1, g2, g3]), ((0, 5), (0, 0)))
    rows = jnp.concatenate([current, gains], axis=0)
    blocks = [rows] + [pull(rows, "x", d) for d in (1, 2, 3)]
    blocks = [jnp.concatenate([b, pull(b, "c", 1)], axis=1) for b in blocks]
    turned = [rolled(b[:length], 1, ((y + 2 * core) % 4) * 128) for b in blocks]
    turned = rolled(jnp.concatenate(turned, axis=1), 1, ((z - x) % 4) * 512)
    some = [
        jnp.concatenate(
            [lax.dynamic_slice_in_dim(b, 48 * tp, 48, 0), b[length : length + 8]], axis=0
        )
        for b in blocks
    ]
    some = [rolled(b, 1, core * 256) for b in some]
    some = rolled(jnp.concatenate(some, axis=1), 1, ((4 - x) % 4) * 512)
    own_rows, gains = some[:48].astype(F32), some[48:51].astype(F32)

    near_gate, near_up = neighbours(gate_part, "y"), neighbours(up_part, "z")
    far_gate, far_up = opposite(*near_gate, "y"), opposite(*near_up, "z")
    gate_of = [
        jnp.concatenate([turned[:, 512 * k + 128 * d :][:, :128] for k in range(4)], axis=1)
        for d in range(4)
    ]
    up_of = [turned[:, 512 * d : 512 * (d + 1)] for d in range(4)]

    def split_sum(left, own, near, far):
        total = matmul(left[0], own)
        total = total + matmul(left[1], near[0])
        total = total + matmul(left[3], near[1])
        total = total + matmul(left[2][:, :256], far[0])
        return total + matmul(left[2][:, 256:], far[1])

    gate = split_sum(gate_of, gate_part, near_gate, far_gate)
    up = split_sum(up_of, up_part, near_up, far_up)
    hidden = (jax.nn.silu(gate) * up).astype(BF16)

    def down(rows_other, rows_own, weight, product=matmul):
        return summed_rows(product(rows_other, weight), product(rows_own, weight))

    branch = down(*by_owner(hidden, x, core), early[:768])
    first = norm_rows(ALPHA * own_rows + 0.5 * branch, gains[0])

    def every_row(rows):
        near, far, near_other, far_other = across(rows)
        return jnp.concatenate([near, far, near_other, far_other], axis=0)

    def by_distance(values):
        count = values.shape[0] // 8
        at = [values[count * k : count * (k + 1)] for k in range(8)]
        own = [at[SIDES.index(d)] for d in range(4)]
        other = [at[4 + SIDES.index(d)] for d in range(4)]
        return own, other

    def gated_linear(rows):
        both = matmul_t(rows, early[896:])
        return both[:, :128] * jax.nn.sigmoid(both[:, 128:])

    gated = in_order(list(zip(*by_distance(gated_linear(every_row(first))))), x, core)
    reach = (conv_taps.shape[0] - 1) // 2
    padded = jnp.pad(gated, ((reach, reach), (0, 0)))
    taps = conv_taps.astype(F32)
    mixed = jnp.zeros_like(gated)
    for k in range(conv_taps.shape[0]):
        mixed = mixed + taps[k] * padded[k : k + length]
    center, spread = channel_stats(mixed)
    normed = (mixed - center) * lax.rsqrt(spread + EPSILON) * conv_gain.astype(F32)
    act = jax.nn.silu(normed).astype(BF16)
    branch = down(*by_owner(act, x, core), early[768:896])
    second = norm_rows(ALPHA * first.astype(F32) + branch, gains[1])

    rows = every_row(second)
    own, other = by_distance(gated_hidden(rows, late, 768))
    branch = down(
        jnp.concatenate(other, axis=0), jnp.concatenate(own, axis=0), late[:, 1536:], matmul_t
    )
    out = norm_rows(ALPHA * second.astype(F32) + 0.5 * branch, gains[2])
    out = out.reshape(-1, 8, 256).transpose(1, 0, 2)
    out = lax.all_to_all(out, "tp", split_axis=0, concat_axis=0, tiled=True)
    return out.reshape(1, -1, 256)


def solution(mesh):
    return jax.shard_map(
        layer,
        mesh=mesh,
        in_specs=(
            P("fs", None, "tp"),
            P("fs", "tp"),
            P("fs", "tp"),
            P("tp", "fs"),
            P("tp"),
            P("fs", "tp"),
            P("fs", "tp"),
            P(None, "tp"),
            P("tp"),
            P("tp", "fs"),
            P("tp"),
            P("fs", "tp"),
            P("fs", "tp"),
            P("tp", "fs"),
            P("tp"),
        ),
        out_specs=P("fs", None, "tp"),
        check_vma=False,
    )
```
